32 devices in a mesh: sp: 16 (over z, y, x), tp: 2 (over core).
Axes of the slice: x: 2, y: 2, z: 4, core: 2. Of those that a mesh axis runs over, the one named last changes fastest.
Arguments:
- stream_mid: bfloat16 [3072, 2048], P('sp'), may hold values from -6 to 6
- d_out: bfloat16 [3072, 2048], P('sp'), may hold values from -6 to 6
- route_ids: int32 [3072, 2], P('sp'), may hold values from 0 to 15, all different within a row; in each aligned block of 192 rows (0 to 191, 192 to 383, ...) at most 48 rows name the same one
- route_weights: float32 [3072, 2], P('sp'), may hold values from 0.3 to 1.5
- gate_pre: bfloat16 [3072, 2048], P('sp', 'tp'), may hold values from -6 to 6
- lru_out: bfloat16 [3072, 2048], P('sp', 'tp'), may hold values from -6 to 6
- log_decay: float32 [3072, 2048], P('sp', 'tp'), may hold values from -2.5 to 0
- w_out: bfloat16 [2048, 2048], P('tp'), may hold values from -0.125 to 0.125
- exp_gate: bfloat16 [16, 2048, 1024], P('sp', None, 'tp'), may hold values from -0.125 to 0.125
- exp_up: bfloat16 [16, 2048, 1024], P('sp', None, 'tp'), may hold values from -0.125 to 0.125
- exp_down: bfloat16 [16, 1024, 2048], P('sp', 'tp'), may hold values from -0.1875 to 0.1875
Outputs:
- grad_exp_gate: float32 [16, 2048, 1024], P('sp', None, 'tp')
- grad_exp_up: float32 [16, 2048, 1024], P('sp', None, 'tp')
- grad_exp_down: float32 [16, 1024, 2048], P('sp', 'tp')
- grad_out_proj: float32 [2048, 2048], P('sp', 'tp')
- d_gate: bfloat16 [3072, 2048], P('sp', 'tp')
- d_drive: float32 [3072, 2048], P('sp', 'tp')
- d_log_decay: float32 [3072, 2048], P('sp', 'tp')
The draws below stay inside these ranges and needn't reach their ends.
Inputs may be any that keep to these rules, and one draw needn't show every extreme that they name: `route_ids`: each row names 2 different experts; among the rows of one index of sp no expert is named by more than 48 rows, and in every draw some expert is named by exactly 48 of them.
All inputs are finite; a program needn't handle non-finite values.
Results may differ from the reference program's by a relative error of at most 0.0069.
Values may be sent and summed in bfloat16 or wider, within the bound.
A program may use at most 128 MiB of HBM per device.

```python
import math
import jax
import jax.numpy as jnp
import numpy as np
from jax import lax

D = 2048
RECURRENT_WIDTH = 2048
FF_E = 1024
TOPK = 2
TOK_DEV = 192
EXPERTS = 16
SEQUENCE_TOKENS = 3072
CAP = 48
N_SP = 16
N_TP = 2


def draw_log_decay(key, part):
    key_sequence = jax.random.split(jax.random.fold_in(key, 71), 7)
    slow_rate = jax.random.uniform(key_sequence[0], (RECURRENT_WIDTH,), jnp.float32, 0.2, 0.6) / SEQUENCE_TOKENS
    fast_rate = jnp.exp(jax.random.uniform(key_sequence[1], (RECURRENT_WIDTH,), jnp.float32, jnp.log(1.0 / 100.0), jnp.log(1.0 / 30.0)))
    slow_mask = jax.random.uniform(key_sequence[2], (RECURRENT_WIDTH,), jnp.float32) < 0.5
    base_rate = jnp.where(slow_mask, slow_rate, fast_rate)
    block_count = SEQUENCE_TOKENS // TOK_DEV
    block_factor = jnp.exp(jax.random.uniform(key_sequence[3], (block_count, 1), jnp.float32, 0.0, jnp.log(2.5)))
    jitter = jnp.exp(jax.random.uniform(key_sequence[4], (SEQUENCE_TOKENS, RECURRENT_WIDTH), jnp.float32, jnp.log(0.5), jnp.log(2.0)))
    decay_speeds = base_rate[None, :] * jnp.repeat(block_factor, TOK_DEV, axis=0) * jitter
    surge_token_rows = jax.random.randint(key_sequence[5], (3,), 0, SEQUENCE_TOKENS)
    surge_token_loss = jax.random.uniform(key_sequence[6], (3, RECURRENT_WIDTH), jnp.float32, 0.2, 0.5)
    surge_token_hit = (jnp.arange(SEQUENCE_TOKENS)[:, None] == surge_token_rows[None, :]).astype(jnp.float32)
    decay_speeds = decay_speeds + jnp.dot(surge_token_hit, -jnp.log(1.0 - surge_token_loss), precision=lax.Precision.HIGHEST)
    return -decay_speeds


def strengthened(result, own_key, source, target, blocks, factor):
    def block_of(axis_at):
        return (jnp.arange(result.shape[axis_at]) // (result.shape[axis_at] // blocks)).reshape((-1,) + (1,) * (result.ndim - 1 - axis_at))

    near = jax.random.permutation(own_key, blocks)[block_of(target)]
    second = (block_of(target) + blocks // 2) % blocks
    return jnp.where((block_of(source) == near) | (block_of(source) == second), factor * result, result)


def steps_of(stream_key, shape, cuts, smallest, top_value):
    factor_of = 1.0
    for axis_at, blocks in cuts:
        steps = jax.random.uniform(jax.random.fold_in(jax.random.fold_in(stream_key, 6), axis_at), (blocks,), jnp.float32, smallest / len(cuts), top_value / len(cuts))
        factor_of = factor_of * jnp.repeat(jnp.exp(steps), shape[axis_at] // blocks).reshape((-1,) + (1,) * (len(shape) - 1 - axis_at))
    return factor_of


def shared_out(rng, own, number, rows, amount, top, limit, slope):
    order = jax.random.permutation(rng, amount)
    packed, usual = load_shares(amount, rows * top, limit, slope, True), load_shares(amount, rows * top, limit, slope, False)
    places = jnp.arange(amount)

    def named(sizes, turn):
        used = int((sizes > 0).sum())
        fixed = max(1, used // 4)
        moved = fixed + (places - fixed + turn * (used - fixed)) % max(1, amount - fixed)
        return jnp.zeros((amount,), jnp.int32).at[order[jnp.where(places < fixed, places, moved)]].set(jnp.asarray(sizes, jnp.int32))

    sizes = jnp.where(number % 4 == 0, named(packed, number // 4), named(usual, number - number // 4 - 1))
    mixed = jax.random.permutation(jax.random.fold_in(own, 3), amount)
    giver, taker = mixed[0:amount // 2 * 2:2], mixed[1:amount // 2 * 2:2]
    room = jnp.minimum(sizes[giver] - 1, limit - sizes[taker]) // 2
    room = jnp.where((giver == order[0]) | (taker == order[0]) | (sizes[taker] == 0), 0, jnp.maximum(room, 0))
    moved = jax.random.randint(jax.random.fold_in(own, 4), (amount // 2,), 0, 1 << 20) % (room + 1)
    sizes = sizes.at[giver].add(-moved).at[taker].add(moved)
    items = jnp.searchsorted(jnp.cumsum(sizes), jnp.arange(rows * top), side="right").astype(jnp.int32)
    grid = items.reshape(top, rows).T
    grid = grid[jax.random.permutation(jax.random.fold_in(own, 1), rows)]
    turn = jax.random.randint(jax.random.fold_in(own, 2), (rows, 1), 0, top)
    return jnp.take_along_axis(grid, (jnp.arange(top)[None, :] + turn) % top, axis=1)


def load_shares(amount, total, bound, slope, full):
    loads = [(1 << 20) // math.isqrt(grade ** slope) + 1 for grade in range(1, amount + 1)]
    largest = bound if full else min(bound, max(-(-total // amount), total * loads[0] // sum(loads)))
    least = 1 if total - largest >= amount - 1 else 0
    given, spare = [largest] + [least] * (amount - 1), total - largest - least * (amount - 1)
    while spare > 0:
        movable = [i for i in range(1, amount) if given[i] < largest] or [i for i in range(1, amount) if given[i] < bound]
        whole, remaining = sum([loads[i] for i in movable]), spare
        for i in movable:
            more = min(bound - given[i], max(1, remaining * loads[i] // whole), spare)
            given[i] = given[i] + more
            spare = spare - more
    return np.array(given)


def noise(rng, shape, deviation, bound, shards=(), kind=jnp.bfloat16):
    drawn = deviation * jax.random.normal(rng, shape, jnp.float32)
    if shards:
        drawn = drawn * steps_of(rng, shape, shards, -0.22, 0.18)
    return jnp.clip(drawn, -bound, bound).astype(kind)


def noise_with(stream_key, extent, spread, most, cuts, heavy, kind=jnp.bfloat16):
    entries = spread * jax.random.normal(stream_key, extent, jnp.float32)
    if cuts:
        entries = entries * steps_of(stream_key, extent, cuts, -0.22, 0.18)
    return jnp.clip(strengthened(entries, jax.random.fold_in(stream_key, 3), *heavy), -most, most).astype(kind)


def setup_inputs(seed: int = 0) -> dict:
    seeds = jax.random.split(jax.random.key(seed), 12)
    stream_mid = noise(seeds[0], (SEQUENCE_TOKENS, D), 1.0, 6.0, ((0, 16),))
    d_out = noise_with(seeds[1], (SEQUENCE_TOKENS, D), 1.0, 6.0, ((0, 16),), (0, 1, 16, 2.0))
    route_ids_keys = jax.random.split(jax.random.fold_in(seeds[2], 1), SEQUENCE_TOKENS // TOK_DEV)
    route_ids_turns = jax.random.permutation(jax.random.fold_in(seeds[2], 3), SEQUENCE_TOKENS // TOK_DEV)
    route_ids = jax.vmap(lambda own, number: shared_out(jax.random.fold_in(seeds[2], 2), own, number, TOK_DEV, EXPERTS, TOPK, CAP, 1))(route_ids_keys, route_ids_turns).reshape((SEQUENCE_TOKENS, TOPK))
    route_weights = jnp.clip(0.3 + 1.2 * jax.random.uniform(seeds[3], (SEQUENCE_TOKENS, TOPK), jnp.float32) ** steps_of(seeds[3], (SEQUENCE_TOKENS, TOPK), ((0, 16),), -0.2, 0.2), 0.3, 1.5)
    gate_pre = noise(seeds[4], (SEQUENCE_TOKENS, RECURRENT_WIDTH), 1.0, 6.0, ((0, 16), (1, 2)))
    lru_out = noise(seeds[5], (SEQUENCE_TOKENS, RECURRENT_WIDTH), 1.0, 6.0, ((0, 16), (1, 2)))
    log_decay = draw_log_decay(jax.random.fold_in(seeds[11], 71), 0)
    w_out = noise(seeds[7], (RECURRENT_WIDTH, D), RECURRENT_WIDTH ** -0.5, 0.125, ((0, 2),))
    exp_gate = noise(seeds[8], (EXPERTS, D, FF_E), D ** -0.5, 0.125, ((0, 16), (2, 2)))
    exp_up = noise(seeds[9], (EXPERTS, D, FF_E), D ** -0.5, 0.125, ((0, 16), (2, 2)))
    exp_down = noise(seeds[10], (EXPERTS, FF_E, D), FF_E ** -0.5, 0.1875, ((0, 16), (1, 2)))
    return {"stream_mid": stream_mid, "d_out": d_out, "route_ids": route_ids, "route_weights": route_weights, "gate_pre": gate_pre, "lru_out": lru_out, "log_decay": log_decay, "w_out": w_out, "exp_gate": exp_gate, "exp_up": exp_up, "exp_down": exp_down}


def reverse_recurrence(decay_rate, drive):
    coeffs = jnp.concatenate([decay_rate[1:], jnp.zeros_like(decay_rate[:1])], axis=0)

    def combine(earlier, later):
        return (earlier[0] * later[0], later[0] * earlier[1] + later[1])
    _, carried = lax.associative_scan(combine, (jnp.flip(coeffs, 0), jnp.flip(drive, 0)), axis=0)
    return jnp.flip(carried, 0)

def contract_rows(left, right):
    return lax.dot_general(left, right, (((0,), (0,)), ((), ())), preferred_element_type=jnp.float32)

def contract_cols(left, right):
    return lax.dot_general(left, right, (((1,), (1,)), ((), ())), preferred_element_type=jnp.float32)

def reference(stream_mid, d_out, route_ids, route_weights, gate_pre, lru_out, log_decay, w_out, exp_gate, exp_up, exp_down):
    token_total = d_out.shape[0]
    slot_total = N_SP * CAP
    half_units = FF_E // N_TP
    flat_ids = route_ids.reshape(-1)
    padded_stream = jnp.concatenate([stream_mid, jnp.zeros((1, D), jnp.bfloat16)], axis=0)
    scaled = (route_weights[:, :, None] * d_out.astype(jnp.float32)[:, None, :]).astype(jnp.bfloat16)
    padded_scaled = jnp.concatenate([scaled.reshape(-1, D), jnp.zeros((1, D), jnp.bfloat16)], axis=0)

    def one_expert(expert):
        found = jnp.nonzero(flat_ids == expert, size=slot_total, fill_value=token_total * TOPK)[0].astype(jnp.int32)
        inputs = padded_stream[found // TOPK]
        cotangent = padded_scaled[found]
        gate_weight = exp_gate[expert]
        up_weight = exp_up[expert]
        down_weight = exp_down[expert]
        gate_proj = jnp.dot(inputs, gate_weight, preferred_element_type=jnp.float32)
        up_proj = jnp.dot(inputs, up_weight, preferred_element_type=jnp.float32)
        gate_sigmoid = jax.nn.sigmoid(gate_proj)
        gate_act = gate_proj * gate_sigmoid
        hidden = (gate_act * up_proj).astype(jnp.bfloat16)
        back_hidden = contract_cols(cotangent, down_weight)
        grad_gate_pre = (back_hidden * up_proj * gate_sigmoid * (1.0 + gate_proj * (1.0 - gate_sigmoid))).astype(jnp.bfloat16)
        grad_up_pre = (back_hidden * gate_act).astype(jnp.bfloat16)
        grad_down = contract_rows(hidden, cotangent)
        grad_gate = contract_rows(inputs, grad_gate_pre)
        grad_up = contract_rows(inputs, grad_up_pre)
        row_sum = jnp.zeros((slot_total, D), jnp.float32)
        for piece in range(N_TP):
            lower = piece * half_units
            upper = lower + half_units
            part_back = contract_cols(grad_gate_pre[:, lower:upper], gate_weight[:, lower:upper])
            part_back = part_back + contract_cols(grad_up_pre[:, lower:upper], up_weight[:, lower:upper])
            rounded = lax.optimization_barrier(part_back.astype(jnp.bfloat16))
            row_sum = row_sum + rounded.astype(jnp.float32)
        return (grad_gate, grad_up, grad_down, row_sum.astype(jnp.bfloat16), found)
    grad_exp_gate, grad_exp_up, grad_exp_down, row_back, found_all = lax.map(one_expert, jnp.arange(EXPERTS, dtype=jnp.int32))
    collected = jnp.zeros((token_total * TOPK + 1, D), jnp.float32)
    collected = collected.at[found_all.reshape(-1)].add(row_back.reshape(-1, D).astype(jnp.float32))
    routed_back = lax.optimization_barrier(jnp.sum(collected[:-1].reshape(token_total, TOPK, D), axis=1))
    d_mid = (d_out.astype(jnp.float32) + routed_back).astype(jnp.bfloat16)
    d_gated = contract_cols(d_mid, w_out)
    state_vals = lru_out.astype(jnp.float32)
    gelu_val, gelu_back = jax.vjp(jax.nn.gelu, gate_pre.astype(jnp.float32))
    gated = (gelu_val * state_vals).astype(jnp.bfloat16)
    grad_out_proj = contract_rows(d_mid, gated)
    d_gate = gelu_back(d_gated * state_vals)[0].astype(jnp.bfloat16)
    decay_rate = jnp.exp(log_decay)
    d_drive = reverse_recurrence(decay_rate, d_gated * gelu_val)
    prev_state = jnp.concatenate([jnp.zeros_like(state_vals[:1]), state_vals[:-1]], axis=0)
    d_log_decay = d_drive * decay_rate * prev_state
    return (grad_exp_gate, grad_exp_up, grad_exp_down, grad_out_proj, d_gate, d_drive, d_log_decay)
```

```python
import functools

import jax
import jax.numpy as jnp
from jax import lax
from jax.experimental import pallas as pl
from jax.experimental.pallas import tpu as pltpu
from jax.sharding import PartitionSpec as P

TOPK = 2
EXP_DEV = 1
GELU_SCALE = 0.7978845608028654
GELU_CUBIC = 0.044715


def shifted(value, axis, steps):
    count = lax.axis_size(axis)
    leading, last = (max(0, -steps), min(count, count - steps))
    return lax.ppermute(value, axis, [(source, source + steps) for source in range(leading, last)])


def swapped(value):
    return lax.ppermute(value, "tp", [(0, 1), (1, 0)])


def contract_rows(left, right):
    return lax.dot_general(
        left, right, (((0,), (0,)), ((), ())), preferred_element_type=jnp.float32
    )


def contract_cols(left, right):
    return lax.dot_general(
        left, right, (((1,), (1,)), ((), ())), preferred_element_type=jnp.float32
    )


def dot(left, right):
    return jnp.dot(left, right, preferred_element_type=jnp.float32)


def gelu_parts(value):
    squared = value * value
    bent = jnp.tanh(GELU_SCALE * (value + GELU_CUBIC * squared * value))
    half = 0.5 * (1.0 + bent)
    slope = half + 0.5 * value * (1.0 - bent * bent) * GELU_SCALE * (
        1.0 + 3.0 * GELU_CUBIC * squared
    )
    return value * half, slope


def local_kernel(mid_ref, w_ref, pre_ref, state_ref, log_ref, gate_ref, grad_ref, coef_ref, edge_ref):
    d_gated = contract_cols(mid_ref[...], w_ref[...])
    value, slope = gelu_parts(pre_ref[...].astype(jnp.float32))
    gate_ref[...] = (d_gated * state_ref[...].astype(jnp.float32) * slope).astype(jnp.bfloat16)
    decay = jnp.exp(log_ref[...])
    rows, width = decay.shape
    grad = d_gated * value
    coef = jnp.concatenate([decay[1:], jnp.ones((1, width), jnp.float32)], axis=0)
    step = 1
    while step < rows:
        later_grad = jnp.concatenate(
            [grad[step:], jnp.zeros((step, width), jnp.float32)], axis=0
        )
        later_coef = jnp.concatenate([coef[step:], jnp.ones((step, width), jnp.float32)], axis=0)
        grad = grad + coef * later_grad
        coef = coef * later_coef
        step *= 2
    grad_ref[...] = grad
    coef_ref[...] = coef
    edge_ref[0:1, :] = decay[0:1] * coef[0:1]
    edge_ref[1:2, :] = decay[0:1] * grad[0:1]


def local_part(d_mid, w_out, gate_pre, lru_out, log_decay):
    rows, model_width = d_mid.shape
    width = lru_out.shape[1]
    block = 256 if width % 256 == 0 else width
    narrow = pl.BlockSpec((rows, block), lambda i: (0, i))
    return pl.pallas_call(
        local_kernel,
        grid=(width // block,),
        in_specs=[
            pl.BlockSpec((rows, model_width), lambda i: (0, 0)),
            pl.BlockSpec((block, model_width), lambda i: (i, 0)),
            narrow,
            narrow,
            narrow,
        ],
        out_specs=[narrow, narrow, narrow, pl.BlockSpec((2, block), lambda i: (0, i))],
        out_shape=[
            jax.ShapeDtypeStruct((rows, width), jnp.bfloat16),
            jax.ShapeDtypeStruct((rows, width), jnp.float32),
            jax.ShapeDtypeStruct((rows, width), jnp.float32),
            jax.ShapeDtypeStruct((2, width), jnp.float32),
        ],
        cost_estimate=pl.CostEstimate(
            flops=2 * rows * width * model_width, bytes_accessed=8 << 20, transcendentals=0
        ),
    )(d_mid, w_out, gate_pre, lru_out, log_decay)


def finish_kernel(count, mine_ref, edges_ref, grad_ref, coef_ref, log_ref, prev_ref, before_ref, drive_ref, out_ref):
    mine = mine_ref[0]
    width = grad_ref.shape[1]
    carry = jnp.zeros((1, width), jnp.float32)
    for position in range(count - 1, 0, -1):
        longer = edges_ref[position, 1:2, :] + edges_ref[position, 0:1, :] * carry
        carry = jnp.where(position > mine, longer, carry)
    drive = grad_ref[...] + coef_ref[...] * carry
    drive_ref[...] = drive
    states = prev_ref[...].astype(jnp.float32)
    prev = jnp.concatenate([before_ref[...].astype(jnp.float32), states[:-1]], axis=0)
    out_ref[...] = drive * jnp.exp(log_ref[...]) * prev


def finish_part(mine, edges, grad, coef, log_decay, lru_out, before_row):
    rows, width = grad.shape
    count = edges.shape[0]
    block = 256 if width % 256 == 0 else width
    narrow = pl.BlockSpec((rows, block), lambda i: (0, i))
    return pl.pallas_call(
        functools.partial(finish_kernel, count),
        grid=(width // block,),
        in_specs=[
            pl.BlockSpec(memory_space=pltpu.SMEM),
            pl.BlockSpec((count, 2, block), lambda i: (0, 0, i)),
            narrow,
            narrow,
            narrow,
            narrow,
            pl.BlockSpec((1, block), lambda i: (0, i)),
        ],
        out_specs=[narrow, narrow],
        out_shape=[jax.ShapeDtypeStruct((rows, width), jnp.float32)] * 2,
        cost_estimate=pl.CostEstimate(
            flops=8 * rows * width, bytes_accessed=5 << 20, transcendentals=0
        ),
    )(mine, edges, grad, coef, log_decay, lru_out, before_row)


def on_device(
    stream_mid,
    d_out,
    route_ids,
    route_weights,
    gate_pre,
    lru_out,
    log_decay,
    w_out,
    exp_gate,
    exp_up,
    exp_down,
):
    rows_local = d_out.shape[0]
    model_width = d_out.shape[1]
    sp_count = lax.axis_size("sp")
    tp_index = lax.axis_index("tp")
    lines = 4 if sp_count % 4 == 0 else 1
    plane = sp_count // lines
    plane_groups = [[line * plane + place for place in range(plane)] for line in range(lines)]
    line_groups = [[line * plane + place for line in range(lines)] for place in range(plane)]
    expert_count = EXP_DEV * sp_count
    capacity = max(2, 2 * rows_local * TOPK // expert_count)
    slot_count = expert_count * capacity
    half_cols = model_width // 2
    own_start = tp_index * half_cols
    other_start = half_cols - own_start

    experts = jnp.arange(expert_count, dtype=jnp.int32)[None, :]
    slots = jnp.arange(slot_count, dtype=jnp.int32)[None, :]
    places = jnp.arange(rows_local, dtype=jnp.int32)
    earlier = (places[None, :] < places[:, None]).astype(jnp.bfloat16)
    hits = []
    before = jnp.zeros((1, expert_count), jnp.float32)
    for pick in range(TOPK):
        chosen = route_ids[:, pick : pick + 1]
        onehot = (chosen == experts).astype(jnp.bfloat16)
        wide = onehot.astype(jnp.float32)
        rank = dot(earlier, onehot) + before
        before = before + jnp.sum(wide, axis=0, keepdims=True)
        place = jnp.sum(rank * wide, axis=1, keepdims=True).astype(jnp.int32)
        hits.append(slots == chosen * capacity + place)
    any_hit = (hits[0] | hits[1]).astype(jnp.bfloat16)
    each_hit = jnp.concatenate([hit.astype(jnp.bfloat16) for hit in hits], axis=0)
    stream_half = lax.dynamic_slice_in_dim(stream_mid, own_start, half_cols, 1)
    cot_half = lax.dynamic_slice_in_dim(d_out, own_start, half_cols, 1)
    cot_wide = cot_half.astype(jnp.float32)
    scaled = jnp.concatenate(
        [
            (route_weights[:, pick : pick + 1] * cot_wide).astype(jnp.bfloat16)
            for pick in range(TOPK)
        ],
        axis=0,
    )
    rows_piece = contract_rows(any_hit, stream_half).astype(jnp.bfloat16)
    cot_piece = contract_rows(each_hit, scaled).astype(jnp.bfloat16)
    rows_piece = rows_piece.reshape(sp_count, EXP_DEV * capacity, half_cols)
    cot_piece = cot_piece.reshape(sp_count, EXP_DEV * capacity, half_cols)
    got_rows = lax.all_to_all(rows_piece, "sp", split_axis=0, concat_axis=0, tiled=True)
    got_cot = lax.all_to_all(cot_piece, "sp", split_axis=0, concat_axis=0, tiled=True)
    inputs = lax.all_gather(got_rows, "tp", axis=2, tiled=True).reshape(slot_count, model_width)
    cotangent = lax.all_gather(got_cot, "tp", axis=2, tiled=True).reshape(slot_count, model_width)

    gate_value, _ = gelu_parts(gate_pre.astype(jnp.float32))
    gated = (gate_value * lru_out.astype(jnp.float32)).astype(jnp.bfloat16)
    plane_gated = lax.all_gather(gated, "sp", axis=0, tiled=True, axis_index_groups=plane_groups)
    before_row = shifted(lru_out[-1:], "sp", 1)

    gate_proj = dot(inputs, exp_gate[0])
    up_proj = dot(inputs, exp_up[0])
    gate_sigmoid = jax.nn.sigmoid(gate_proj)
    gate_act = gate_proj * gate_sigmoid
    hidden = (gate_act * up_proj).astype(jnp.bfloat16)
    back_hidden = contract_cols(cotangent, exp_down[0])
    grad_gate_pre = (
        back_hidden * up_proj * gate_sigmoid * (1.0 + gate_proj * (1.0 - gate_sigmoid))
    ).astype(jnp.bfloat16)
    grad_up_pre = (back_hidden * gate_act).astype(jnp.bfloat16)

    def back_piece(start):
        gate_rows = lax.dynamic_slice_in_dim(exp_gate[0], start, half_cols, 0)
        up_rows = lax.dynamic_slice_in_dim(exp_up[0], start, half_cols, 0)
        piece = contract_cols(grad_gate_pre, gate_rows) + contract_cols(grad_up_pre, up_rows)
        return piece.astype(jnp.bfloat16)

    from_other = swapped(back_piece(other_start))
    own_piece = back_piece(own_start)
    summed_back = (own_piece.astype(jnp.float32) + from_other.astype(jnp.float32)).astype(
        jnp.bfloat16
    )
    summed_back = summed_back.reshape(sp_count, EXP_DEV * capacity, half_cols)
    returned = lax.all_to_all(summed_back, "sp", split_axis=0, concat_axis=0, tiled=True)
    routed_back = dot(any_hit, returned.reshape(slot_count, half_cols))
    mid_half = (cot_wide + routed_back).astype(jnp.bfloat16)
    mid_other = swapped(mid_half)
    first = tp_index == 0
    d_mid = jnp.concatenate(
        [jnp.where(first, mid_half, mid_other), jnp.where(first, mid_other, mid_half)], axis=1
    )

    down_grad = contract_rows(hidden, cotangent)
    gate_grad = contract_rows(inputs, grad_gate_pre)
    up_grad = contract_rows(inputs, grad_up_pre)

    share = model_width // sp_count
    mid_pieces = jnp.stack(
        [
            jnp.concatenate(
                [
                    d_mid[:, (line * plane + place) * share : (line * plane + place + 1) * share]
                    for line in range(lines)
                ],
                axis=1,
            )
            for place in range(plane)
        ],
        axis=0,
    )
    mid_pieces = lax.all_to_all(
        mid_pieces, "sp", split_axis=0, concat_axis=0, tiled=True, axis_index_groups=plane_groups
    )
    mid_rows = mid_pieces.reshape(plane * rows_local, lines * share)
    partial = contract_rows(mid_rows, plane_gated).astype(jnp.bfloat16)
    grad_out_proj = lax.psum_scatter(
        partial, "sp", scatter_dimension=0, tiled=True, axis_index_groups=line_groups
    ).astype(jnp.float32)

    d_gate, local_grad, coef, edge = local_part(d_mid, w_out, gate_pre, lru_out, log_decay)
    edges = lax.all_gather(edge, "sp")
    mine = lax.axis_index("sp").reshape(1).astype(jnp.int32)
    d_drive, d_log_decay = finish_part(
        mine, edges, local_grad, coef, log_decay, lru_out, before_row
    )
    return (
        gate_grad[None],
        up_grad[None],
        down_grad[None],
        grad_out_proj,
        d_gate,
        d_drive,
        d_log_decay,
    )


def solution(mesh):
    in_specs = (
        P("sp", None),
        P("sp", None),
        P("sp", None),
        P("sp", None),
        P("sp", "tp"),
        P("sp", "tp"),
        P("sp", "tp"),
        P("tp", None),
        P("sp", None, "tp"),
        P("sp", None, "tp"),
        P("sp", "tp", None),
    )
    out_specs = (
        P("sp", None, "tp"),
        P("sp", None, "tp"),
        P("sp", "tp", None),
        P("sp", "tp"),
        P("sp", "tp"),
        P("sp", "tp"),
        P("sp", "tp"),
    )
    return jax.shard_map(
        on_device, mesh=mesh, in_specs=in_specs, out_specs=out_specs, check_vma=False
    )
```

```python
import functools

import jax
import jax.numpy as jnp
from jax import lax
from jax.experimental import pallas as pl
from jax.experimental.pallas import tpu as pltpu
from jax.sharding import PartitionSpec as P

TOPK = 2
EXP_DEV = 1
GELU_SCALE = 0.7978845608028654
GELU_CUBIC = 0.044715


def shifted(value, axis, steps):
    count = lax.axis_size(axis)
    leading, last = (max(0, -steps), min(count, count - steps))
    return lax.ppermute(value, axis, [(source, source + steps) for source in range(leading, last)])


def swapped(value):
    return lax.ppermute(value, "tp", [(0, 1), (1, 0)])


def contract_rows(left, right):
    return lax.dot_general(
        left, right, (((0,), (0,)), ((), ())), preferred_element_type=jnp.float32
    )


def contract_cols(left, right):
    return lax.dot_general(
        left, right, (((1,), (1,)), ((), ())), preferred_element_type=jnp.float32
    )


def dot(left, right):
    return jnp.dot(left, right, preferred_element_type=jnp.float32)


def gelu_parts(value):
    squared = value * value
    bent = jnp.tanh(GELU_SCALE * (value + GELU_CUBIC * squared * value))
    half = 0.5 * (1.0 + bent)
    slope = half + 0.5 * value * (1.0 - bent * bent) * GELU_SCALE * (
        1.0 + 3.0 * GELU_CUBIC * squared
    )
    return value * half, slope


def local_kernel(mid_ref, w_ref, pre_ref, state_ref, log_ref, gate_ref, grad_ref, coef_ref, edge_ref):
    d_gated = contract_cols(mid_ref[...], w_ref[...])
    value, slope = gelu_parts(pre_ref[...].astype(jnp.float32))
    gate_ref[...] = (d_gated * state_ref[...].astype(jnp.float32) * slope).astype(jnp.bfloat16)
    decay = jnp.exp(log_ref[...])
    rows, width = decay.shape
    grad = d_gated * value
    coef = jnp.concatenate([decay[1:], jnp.ones((1, width), jnp.float32)], axis=0)
    step = 1
    while step < rows:
        later_grad = jnp.concatenate(
            [grad[step:], jnp.zeros((step, width), jnp.float32)], axis=0
        )
        later_coef = jnp.concatenate([coef[step:], jnp.ones((step, width), jnp.float32)], axis=0)
        grad = grad + coef * later_grad
        coef = coef * later_coef
        step *= 2
    grad_ref[...] = grad
    coef_ref[...] = coef
    edge_ref[0:1, :] = decay[0:1] * coef[0:1]
    edge_ref[1:2, :] = decay[0:1] * grad[0:1]


def local_part(d_mid, w_out, gate_pre, lru_out, log_decay):
    rows, model_width = d_mid.shape
    width = lru_out.shape[1]
    block = 256 if width % 256 == 0 else width
    narrow = pl.BlockSpec((rows, block), lambda i: (0, i))
    return pl.pallas_call(
        local_kernel,
        grid=(width // block,),
        in_specs=[
            pl.BlockSpec((rows, model_width), lambda i: (0, 0)),
            pl.BlockSpec((block, model_width), lambda i: (i, 0)),
            narrow,
            narrow,
            narrow,
        ],
        out_specs=[narrow, narrow, narrow, pl.BlockSpec((2, block), lambda i: (0, i))],
        out_shape=[
            jax.ShapeDtypeStruct((rows, width), jnp.bfloat16),
            jax.ShapeDtypeStruct((rows, width), jnp.float32),
            jax.ShapeDtypeStruct((rows, width), jnp.float32),
            jax.ShapeDtypeStruct((2, width), jnp.float32),
        ],
        cost_estimate=pl.CostEstimate(
            flops=2 * rows * width * model_width, bytes_accessed=8 << 20, transcendentals=0
        ),
    )(d_mid, w_out, gate_pre, lru_out, log_decay)


def finish_kernel(count, mine_ref, edges_ref, grad_ref, coef_ref, log_ref, prev_ref, before_ref, drive_ref, out_ref):
    mine = mine_ref[0]
    width = grad_ref.shape[1]
    carry = jnp.zeros((1, width), jnp.float32)
    for position in range(count - 1, 0, -1):
        longer = edges_ref[position, 1:2, :] + edges_ref[position, 0:1, :] * carry
        carry = jnp.where(position > mine, longer, carry)
    drive = grad_ref[...] + coef_ref[...] * carry
    drive_ref[...] = drive
    states = prev_ref[...].astype(jnp.float32)
    prev = jnp.concatenate([before_ref[...].astype(jnp.float32), states[:-1]], axis=0)
    out_ref[...] = drive * jnp.exp(log_ref[...]) * prev


def finish_part(mine, edges, grad, coef, log_decay, lru_out, before_row):
    rows, width = grad.shape
    count = edges.shape[0]
    block = 256 if width % 256 == 0 else width
    narrow = pl.BlockSpec((rows, block), lambda i: (0, i))
    return pl.pallas_call(
        functools.partial(finish_kernel, count),
        grid=(width // block,),
        in_specs=[
            pl.BlockSpec(memory_space=pltpu.SMEM),
            pl.BlockSpec((count, 2, block), lambda i: (0, 0, i)),
            narrow,
            narrow,
            narrow,
            narrow,
            pl.BlockSpec((1, block), lambda i: (0, i)),
        ],
        out_specs=[narrow, narrow],
        out_shape=[jax.ShapeDtypeStruct((rows, width), jnp.float32)] * 2,
        cost_estimate=pl.CostEstimate(
            flops=8 * rows * width, bytes_accessed=5 << 20, transcendentals=0
        ),
    )(mine, edges, grad, coef, log_decay, lru_out, before_row)


def spread_kernel(count, edge_ref, out_ref, send_sems, recv_sems):
    mine = lax.axis_index("sp")
    barrier = pltpu.get_barrier_semaphore()
    for step in range(1, count):
        pl.semaphore_signal(
            barrier,
            inc=1,
            device_id={"sp": lax.rem(mine + step, count)},
            device_id_type=pl.DeviceIdType.MESH,
        )
    out_ref[mine] = edge_ref[...]
    pl.semaphore_wait(barrier, count - 1)
    copies = []
    for step in range(1, count):
        copy = pltpu.make_async_remote_copy(
            src_ref=edge_ref,
            dst_ref=out_ref.at[mine],
            send_sem=send_sems.at[step - 1],
            recv_sem=recv_sems.at[step - 1],
            device_id={"sp": lax.rem(mine + step, count)},
            device_id_type=pl.DeviceIdType.MESH,
        )
        copy.start()
        copies.append(copy)
    for copy in copies:
        copy.wait()


def spread_edges(edge):
    count = lax.axis_size("sp")
    return pl.pallas_call(
        functools.partial(spread_kernel, count),
        out_shape=jax.ShapeDtypeStruct((count,) + edge.shape, edge.dtype),
        in_specs=[pl.BlockSpec(memory_space=pltpu.VMEM)],
        out_specs=pl.BlockSpec(memory_space=pltpu.VMEM),
        scratch_shapes=[
            pltpu.SemaphoreType.DMA((count - 1,)),
            pltpu.SemaphoreType.DMA((count - 1,)),
        ],
        compiler_params=pltpu.CompilerParams(collective_id=0, has_side_effects=True),
        cost_estimate=pl.CostEstimate(flops=0, bytes_accessed=16 << 20, transcendentals=0),
    )(edge)


def on_device(
    stream_mid,
    d_out,
    route_ids,
    route_weights,
    gate_pre,
    lru_out,
    log_decay,
    w_out,
    exp_gate,
    exp_up,
    exp_down,
):
    rows_local = d_out.shape[0]
    model_width = d_out.shape[1]
    sp_count = lax.axis_size("sp")
    tp_index = lax.axis_index("tp")
    lines = 4 if sp_count % 4 == 0 else 1
    plane = sp_count // lines
    plane_groups = [[line * plane + place for place in range(plane)] for line in range(lines)]
    line_groups = [[line * plane + place for line in range(lines)] for place in range(plane)]
    expert_count = EXP_DEV * sp_count
    capacity = max(2, 2 * rows_local * TOPK // expert_count)
    slot_count = expert_count * capacity
    half_cols = model_width // 2
    own_start = tp_index * half_cols
    other_start = half_cols - own_start

    experts = jnp.arange(expert_count, dtype=jnp.int32)[None, :]
    slots = jnp.arange(slot_count, dtype=jnp.int32)[None, :]
    places = jnp.arange(rows_local, dtype=jnp.int32)
    earlier = (places[None, :] < places[:, None]).astype(jnp.bfloat16)
    hits = []
    before = jnp.zeros((1, expert_count), jnp.float32)
    for pick in range(TOPK):
        chosen = route_ids[:, pick : pick + 1]
        onehot = (chosen == experts).astype(jnp.bfloat16)
        wide = onehot.astype(jnp.float32)
        rank = dot(earlier, onehot) + before
        before = before + jnp.sum(wide, axis=0, keepdims=True)
        place = jnp.sum(rank * wide, axis=1, keepdims=True).astype(jnp.int32)
        hits.append(slots == chosen * capacity + place)
    any_hit = (hits[0] | hits[1]).astype(jnp.bfloat16)
    each_hit = jnp.concatenate([hit.astype(jnp.bfloat16) for hit in hits], axis=0)
    stream_half = lax.dynamic_slice_in_dim(stream_mid, own_start, half_cols, 1)
    cot_half = lax.dynamic_slice_in_dim(d_out, own_start, half_cols, 1)
    cot_wide = cot_half.astype(jnp.float32)
    scaled = jnp.concatenate(
        [
            (route_weights[:, pick : pick + 1] * cot_wide).astype(jnp.bfloat16)
            for pick in range(TOPK)
        ],
        axis=0,
    )
    rows_piece = contract_rows(any_hit, stream_half).astype(jnp.bfloat16)
    cot_piece = contract_rows(each_hit, scaled).astype(jnp.bfloat16)
    rows_piece = rows_piece.reshape(sp_count, EXP_DEV * capacity, half_cols)
    cot_piece = cot_piece.reshape(sp_count, EXP_DEV * capacity, half_cols)
    got_rows = lax.all_to_all(rows_piece, "sp", split_axis=0, concat_axis=0, tiled=True)
    got_cot = lax.all_to_all(cot_piece, "sp", split_axis=0, concat_axis=0, tiled=True)
    inputs = lax.all_gather(got_rows, "tp", axis=2, tiled=True).reshape(slot_count, model_width)
    cotangent = lax.all_gather(got_cot, "tp", axis=2, tiled=True).reshape(slot_count, model_width)

    gate_value, _ = gelu_parts(gate_pre.astype(jnp.float32))
    gated = (gate_value * lru_out.astype(jnp.float32)).astype(jnp.bfloat16)
    plane_gated = lax.all_gather(gated, "sp", axis=0, tiled=True, axis_index_groups=plane_groups)
    before_row = shifted(lru_out[-1:], "sp", 1)

    gate_proj = dot(inputs, exp_gate[0])
    up_proj = dot(inputs, exp_up[0])
    gate_sigmoid = jax.nn.sigmoid(gate_proj)
    gate_act = gate_proj * gate_sigmoid
    hidden = (gate_act * up_proj).astype(jnp.bfloat16)
    back_hidden = contract_cols(cotangent, exp_down[0])
    grad_gate_pre = (
        back_hidden * up_proj * gate_sigmoid * (1.0 + gate_proj * (1.0 - gate_sigmoid))
    ).astype(jnp.bfloat16)
    grad_up_pre = (back_hidden * gate_act).astype(jnp.bfloat16)

    def back_piece(start):
        gate_rows = lax.dynamic_slice_in_dim(exp_gate[0], start, half_cols, 0)
        up_rows = lax.dynamic_slice_in_dim(exp_up[0], start, half_cols, 0)
        piece = contract_cols(grad_gate_pre, gate_rows) + contract_cols(grad_up_pre, up_rows)
        return piece.astype(jnp.bfloat16)

    from_other = swapped(back_piece(other_start))
    own_piece = back_piece(own_start)
    summed_back = (own_piece.astype(jnp.float32) + from_other.astype(jnp.float32)).astype(
        jnp.bfloat16
    )
    summed_back = summed_back.reshape(sp_count, EXP_DEV * capacity, half_cols)
    returned = lax.all_to_all(summed_back, "sp", split_axis=0, concat_axis=0, tiled=True)
    routed_back = dot(any_hit, returned.reshape(slot_count, half_cols))
    mid_half = (cot_wide + routed_back).astype(jnp.bfloat16)
    mid_other = swapped(mid_half)
    first = tp_index == 0
    d_mid = jnp.concatenate(
        [jnp.where(first, mid_half, mid_other), jnp.where(first, mid_other, mid_half)], axis=1
    )

    down_grad = contract_rows(hidden, cotangent)
    gate_grad = contract_rows(inputs, grad_gate_pre)
    up_grad = contract_rows(inputs, grad_up_pre)

    share = model_width // sp_count
    mid_pieces = jnp.stack(
        [
            jnp.concatenate(
                [
                    d_mid[:, (line * plane + place) * share : (line * plane + place + 1) * share]
                    for line in range(lines)
                ],
                axis=1,
            )
            for place in range(plane)
        ],
        axis=0,
    )
    mid_pieces = lax.all_to_all(
        mid_pieces, "sp", split_axis=0, concat_axis=0, tiled=True, axis_index_groups=plane_groups
    )
    mid_rows = mid_pieces.reshape(plane * rows_local, lines * share)
    partial = contract_rows(mid_rows, plane_gated).astype(jnp.bfloat16)
    grad_out_proj = lax.psum_scatter(
        partial, "sp", scatter_dimension=0, tiled=True, axis_index_groups=line_groups
    ).astype(jnp.float32)

    d_gate, local_grad, coef, edge = local_part(d_mid, w_out, gate_pre, lru_out, log_decay)
    edges = spread_edges(edge)
    mine = lax.axis_index("sp").reshape(1).astype(jnp.int32)
    d_drive, d_log_decay = finish_part(
        mine, edges, local_grad, coef, log_decay, lru_out, before_row
    )
    return (
        gate_grad[None],
        up_grad[None],
        down_grad[None],
        grad_out_proj,
        d_gate,
        d_drive,
        d_log_decay,
    )


def solution(mesh):
    in_specs = (
        P("sp", None),
        P("sp", None),
        P("sp", None),
        P("sp", None),
        P("sp", "tp"),
        P("sp", "tp"),
        P("sp", "tp"),
        P("tp", None),
        P("sp", None, "tp"),
        P("sp", None, "tp"),
        P("sp", "tp", None),
    )
    out_specs = (
        P("sp", None, "tp"),
        P("sp", None, "tp"),
        P("sp", "tp", None),
        P("sp", "tp"),
        P("sp", "tp"),
        P("sp", "tp"),
        P("sp", "tp"),
    )
    return jax.shard_map(
        on_device, mesh=mesh, in_specs=in_specs, out_specs=out_specs, check_vma=False
    )
```

```python
import functools

import jax
import jax.numpy as jnp
from jax import lax
from jax.experimental import pallas as pl
from jax.experimental.pallas import tpu as pltpu
from jax.sharding import PartitionSpec as P

TOPK = 2
EXP_DEV = 1
GELU_SCALE = 0.7978845608028654
GELU_CUBIC = 0.044715


def shifted(value, axis, steps):
    count = lax.axis_size(axis)
    leading, last = (max(0, -steps), min(count, count - steps))
    return lax.ppermute(value, axis, [(source, source + steps) for source in range(leading, last)])


def swapped(value):
    return lax.ppermute(value, "tp", [(0, 1), (1, 0)])


def contract_rows(left, right):
    return lax.dot_general(
        left, right, (((0,), (0,)), ((), ())), preferred_element_type=jnp.float32
    )


def contract_cols(left, right):
    return lax.dot_general(
        left, right, (((1,), (1,)), ((), ())), preferred_element_type=jnp.float32
    )


def dot(left, right):
    return jnp.dot(left, right, preferred_element_type=jnp.float32)


def gelu_parts(value):
    squared = value * value
    bent = jnp.tanh(GELU_SCALE * (value + GELU_CUBIC * squared * value))
    half = 0.5 * (1.0 + bent)
    slope = half + 0.5 * value * (1.0 - bent * bent) * GELU_SCALE * (
        1.0 + 3.0 * GELU_CUBIC * squared
    )
    return value * half, slope


def local_kernel(mid_ref, w_ref, pre_ref, state_ref, log_ref, gate_ref, grad_ref, coef_ref, edge_ref):
    d_gated = contract_cols(mid_ref[...], w_ref[...])
    value, slope = gelu_parts(pre_ref[...].astype(jnp.float32))
    gate_ref[...] = (d_gated * state_ref[...].astype(jnp.float32) * slope).astype(jnp.bfloat16)
    decay = jnp.exp(log_ref[...])
    rows, width = decay.shape
    grad = d_gated * value
    coef = jnp.concatenate([decay[1:], jnp.ones((1, width), jnp.float32)], axis=0)
    step = 1
    while step < rows:
        later_grad = jnp.concatenate(
            [grad[step:], jnp.zeros((step, width), jnp.float32)], axis=0
        )
        later_coef = jnp.concatenate([coef[step:], jnp.ones((step, width), jnp.float32)], axis=0)
        grad = grad + coef * later_grad
        coef = coef * later_coef
        step *= 2
    grad_ref[...] = grad
    coef_ref[...] = coef
    edge_ref[0:1, :] = decay[0:1] * coef[0:1]
    edge_ref[1:2, :] = decay[0:1] * grad[0:1]


def local_part(d_mid, w_out, gate_pre, lru_out, log_decay):
    rows, model_width = d_mid.shape
    width = lru_out.shape[1]
    block = 256 if width % 256 == 0 else width
    narrow = pl.BlockSpec((rows, block), lambda i: (0, i))
    return pl.pallas_call(
        local_kernel,
        grid=(width // block,),
        in_specs=[
            pl.BlockSpec((rows, model_width), lambda i: (0, 0)),
            pl.BlockSpec((block, model_width), lambda i: (i, 0)),
            narrow,
            narrow,
            narrow,
        ],
        out_specs=[narrow, narrow, narrow, pl.BlockSpec((2, block), lambda i: (0, i))],
        out_shape=[
            jax.ShapeDtypeStruct((rows, width), jnp.bfloat16),
            jax.ShapeDtypeStruct((rows, width), jnp.float32),
            jax.ShapeDtypeStruct((rows, width), jnp.float32),
            jax.ShapeDtypeStruct((2, width), jnp.float32),
        ],
        cost_estimate=pl.CostEstimate(
            flops=2 * rows * width * model_width, bytes_accessed=8 << 20, transcendentals=0
        ),
    )(d_mid, w_out, gate_pre, lru_out, log_decay)


def finish_kernel(count, mine_ref, edges_ref, grad_ref, coef_ref, log_ref, prev_ref, before_ref, drive_ref, out_ref):
    mine = mine_ref[0]
    width = grad_ref.shape[1]
    carry = jnp.zeros((1, width), jnp.float32)
    for position in range(count - 1, 0, -1):
        longer = edges_ref[position, 1:2, :] + edges_ref[position, 0:1, :] * carry
        carry = jnp.where(position > mine, longer, carry)
    drive = grad_ref[...] + coef_ref[...] * carry
    drive_ref[...] = drive
    states = prev_ref[...].astype(jnp.float32)
    prev = jnp.concatenate([before_ref[...].astype(jnp.float32), states[:-1]], axis=0)
    out_ref[...] = drive * jnp.exp(log_ref[...]) * prev


def finish_part(mine, edges, grad, coef, log_decay, lru_out, before_row):
    rows, width = grad.shape
    count = edges.shape[0]
    block = 256 if width % 256 == 0 else width
    narrow = pl.BlockSpec((rows, block), lambda i: (0, i))
    return pl.pallas_call(
        functools.partial(finish_kernel, count),
        grid=(width // block,),
        in_specs=[
            pl.BlockSpec(memory_space=pltpu.SMEM),
            pl.BlockSpec((count, 2, block), lambda i: (0, 0, i)),
            narrow,
            narrow,
            narrow,
            narrow,
            pl.BlockSpec((1, block), lambda i: (0, i)),
        ],
        out_specs=[narrow, narrow],
        out_shape=[jax.ShapeDtypeStruct((rows, width), jnp.float32)] * 2,
        cost_estimate=pl.CostEstimate(
            flops=8 * rows * width, bytes_accessed=5 << 20, transcendentals=0
        ),
    )(mine, edges, grad, coef, log_decay, lru_out, before_row)


def spread_kernel(count, edge_ref, out_ref, send_sems, recv_sems):
    mine = lax.axis_index("sp")
    barrier = pltpu.get_barrier_semaphore()
    for step in range(1, count):
        pl.semaphore_signal(
            barrier,
            inc=1,
            device_id={"sp": lax.rem(mine + step, count)},
            device_id_type=pl.DeviceIdType.MESH,
        )
    out_ref[mine] = edge_ref[...]
    pl.semaphore_wait(barrier, count - 1)
    copies = []
    for step in range(1, count):
        copy = pltpu.make_async_remote_copy(
            src_ref=edge_ref,
            dst_ref=out_ref.at[mine],
            send_sem=send_sems.at[step - 1],
            recv_sem=recv_sems.at[step - 1],
            device_id={"sp": lax.rem(mine + step, count)},
            device_id_type=pl.DeviceIdType.MESH,
        )
        copy.start()
        copies.append(copy)
    for copy in copies:
        copy.wait()


def spread_edges(edge):
    count = lax.axis_size("sp")
    return pl.pallas_call(
        functools.partial(spread_kernel, count),
        out_shape=jax.ShapeDtypeStruct((count,) + edge.shape, edge.dtype),
        in_specs=[pl.BlockSpec(memory_space=pltpu.VMEM)],
        out_specs=pl.BlockSpec(memory_space=pltpu.VMEM),
        scratch_shapes=[
            pltpu.SemaphoreType.DMA((count - 1,)),
            pltpu.SemaphoreType.DMA((count - 1,)),
        ],
        compiler_params=pltpu.CompilerParams(collective_id=0, has_side_effects=True),
        cost_estimate=pl.CostEstimate(flops=0, bytes_accessed=16 << 20, transcendentals=0),
    )(edge)


def on_device(
    stream_mid,
    d_out,
    route_ids,
    route_weights,
    gate_pre,
    lru_out,
    log_decay,
    w_out,
    exp_gate,
    exp_up,
    exp_down,
):
    rows_local = d_out.shape[0]
    model_width = d_out.shape[1]
    sp_count = lax.axis_size("sp")
    tp_index = lax.axis_index("tp")
    lines = 4 if sp_count % 4 == 0 else 1
    plane = sp_count // lines
    plane_groups = [[line * plane + place for place in range(plane)] for line in range(lines)]
    line_groups = [[line * plane + place for line in range(lines)] for place in range(plane)]
    expert_count = EXP_DEV * sp_count
    capacity = max(2, 2 * rows_local * TOPK // expert_count)
    slot_count = expert_count * capacity
    half_cols = model_width // 2
    own_start = tp_index * half_cols
    other_start = half_cols - own_start

    experts = jnp.arange(expert_count, dtype=jnp.int32)[None, :]
    slots = jnp.arange(slot_count, dtype=jnp.int32)[None, :]
    places = jnp.arange(rows_local, dtype=jnp.int32)
    earlier = (places[None, :] < places[:, None]).astype(jnp.bfloat16)
    hits = []
    before = jnp.zeros((1, expert_count), jnp.float32)
    for pick in range(TOPK):
        chosen = route_ids[:, pick : pick + 1]
        onehot = (chosen == experts).astype(jnp.bfloat16)
        wide = onehot.astype(jnp.float32)
        rank = dot(earlier, onehot) + before
        before = before + jnp.sum(wide, axis=0, keepdims=True)
        place = jnp.sum(rank * wide, axis=1, keepdims=True).astype(jnp.int32)
        hits.append(slots == chosen * capacity + place)
    any_hit = (hits[0] | hits[1]).astype(jnp.bfloat16)
    stream_half = lax.dynamic_slice_in_dim(stream_mid, own_start, half_cols, 1)
    cot_half = lax.dynamic_slice_in_dim(d_out, own_start, half_cols, 1)
    cot_wide = cot_half.astype(jnp.float32)

    def line_gather(value):
        return lax.all_gather(value, "sp", axis=0, tiled=True, axis_index_groups=line_groups)

    line_stream = line_gather(stream_half)
    line_cot = line_gather(cot_half)
    routes = line_gather(jnp.concatenate([route_ids.astype(jnp.float32), route_weights], axis=1))
    plane_start = lax.axis_index("sp") // plane * plane
    locals_ = jnp.arange(plane, dtype=jnp.int32)[None, :]
    plane_slots = jnp.arange(plane * capacity, dtype=jnp.int32)[None, :]
    row_blocks, cot_blocks = ([], [])
    for line in range(lines):
        block = slice(line * rows_local, (line + 1) * rows_local)
        block_cot = line_cot[block].astype(jnp.float32)
        block_hits, block_scaled = ([], [])
        before = jnp.zeros((1, plane), jnp.float32)
        for pick in range(TOPK):
            chosen = routes[block, pick : pick + 1].astype(jnp.int32) - plane_start
            onehot = (chosen == locals_).astype(jnp.bfloat16)
            wide = onehot.astype(jnp.float32)
            rank = dot(earlier, onehot) + before
            before = before + jnp.sum(wide, axis=0, keepdims=True)
            place = jnp.sum(rank * wide, axis=1, keepdims=True).astype(jnp.int32)
            block_hits.append(plane_slots == chosen * capacity + place)
            weight = routes[block, TOPK + pick : TOPK + pick + 1]
            block_scaled.append((weight * block_cot).astype(jnp.bfloat16))
        block_any = (block_hits[0] | block_hits[1]).astype(jnp.bfloat16)
        block_each = jnp.concatenate([hit.astype(jnp.bfloat16) for hit in block_hits], axis=0)
        shape = (plane, 1, capacity, half_cols)
        row_blocks.append(
            contract_rows(block_any, line_stream[block]).astype(jnp.bfloat16).reshape(shape)
        )
        cot_blocks.append(
            contract_rows(block_each, jnp.concatenate(block_scaled, axis=0))
            .astype(jnp.bfloat16)
            .reshape(shape)
        )

    def plane_exchange(blocks):
        pieces = jnp.concatenate(blocks, axis=1).reshape(plane, lines * capacity, half_cols)
        return lax.all_to_all(
            pieces, "sp", split_axis=0, concat_axis=0, tiled=True, axis_index_groups=plane_groups
        )

    got_rows = plane_exchange(row_blocks)
    got_cot = plane_exchange(cot_blocks)
    inputs = lax.all_gather(got_rows, "tp", axis=2, tiled=True).reshape(slot_count, model_width)
    cotangent = lax.all_gather(got_cot, "tp", axis=2, tiled=True).reshape(slot_count, model_width)

    gate_value, _ = gelu_parts(gate_pre.astype(jnp.float32))
    gated = (gate_value * lru_out.astype(jnp.float32)).astype(jnp.bfloat16)
    plane_gated = lax.all_gather(gated, "sp", axis=0, tiled=True, axis_index_groups=plane_groups)
    before_row = shifted(lru_out[-1:], "sp", 1)

    gate_proj = dot(inputs, exp_gate[0])
    up_proj = dot(inputs, exp_up[0])
    gate_sigmoid = jax.nn.sigmoid(gate_proj)
    gate_act = gate_proj * gate_sigmoid
    hidden = (gate_act * up_proj).astype(jnp.bfloat16)
    back_hidden = contract_cols(cotangent, exp_down[0])
    grad_gate_pre = (
        back_hidden * up_proj * gate_sigmoid * (1.0 + gate_proj * (1.0 - gate_sigmoid))
    ).astype(jnp.bfloat16)
    grad_up_pre = (back_hidden * gate_act).astype(jnp.bfloat16)

    def back_piece(start):
        gate_rows = lax.dynamic_slice_in_dim(exp_gate[0], start, half_cols, 0)
        up_rows = lax.dynamic_slice_in_dim(exp_up[0], start, half_cols, 0)
        piece = contract_cols(grad_gate_pre, gate_rows) + contract_cols(grad_up_pre, up_rows)
        return piece.astype(jnp.bfloat16)

    from_other = swapped(back_piece(other_start))
    own_piece = back_piece(own_start)
    summed_back = (own_piece.astype(jnp.float32) + from_other.astype(jnp.float32)).astype(
        jnp.bfloat16
    )
    summed_back = summed_back.reshape(plane, lines, capacity, half_cols).transpose(1, 0, 2, 3)
    summed_back = summed_back.reshape(sp_count, EXP_DEV * capacity, half_cols)
    returned = lax.all_to_all(summed_back, "sp", split_axis=0, concat_axis=0, tiled=True)
    down_grad = contract_rows(hidden, cotangent)
    gate_grad = contract_rows(inputs, grad_gate_pre)
    up_grad = contract_rows(inputs, grad_up_pre)
    returned, down_grad, gate_grad, up_grad = lax.optimization_barrier(
        (returned, down_grad, gate_grad, up_grad)
    )
    routed_back = dot(any_hit, returned.reshape(slot_count, half_cols))
    mid_half = (cot_wide + routed_back).astype(jnp.bfloat16)
    mid_other = swapped(mid_half)
    first = tp_index == 0
    d_mid = jnp.concatenate(
        [jnp.where(first, mid_half, mid_other), jnp.where(first, mid_other, mid_half)], axis=1
    )

    share = model_width // sp_count
    mid_pieces = jnp.stack(
        [
            jnp.concatenate(
                [
                    d_mid[:, (line * plane + place) * share : (line * plane + place + 1) * share]
                    for line in range(lines)
                ],
                axis=1,
            )
            for place in range(plane)
        ],
        axis=0,
    )
    mid_pieces = lax.all_to_all(
        mid_pieces, "sp", split_axis=0, concat_axis=0, tiled=True, axis_index_groups=plane_groups
    )
    d_gate, local_grad, coef, edge = local_part(d_mid, w_out, gate_pre, lru_out, log_decay)
    mid_pieces, edge = lax.optimization_barrier((mid_pieces, edge))
    mid_rows = mid_pieces.reshape(plane * rows_local, lines * share)
    partial = contract_rows(mid_rows, plane_gated).astype(jnp.bfloat16)
    grad_out_proj = lax.psum_scatter(
        partial, "sp", scatter_dimension=0, tiled=True, axis_index_groups=line_groups
    ).astype(jnp.float32)

    edges = spread_edges(edge)
    mine = lax.axis_index("sp").reshape(1).astype(jnp.int32)
    d_drive, d_log_decay = finish_part(
        mine, edges, local_grad, coef, log_decay, lru_out, before_row
    )
    return (
        gate_grad[None],
        up_grad[None],
        down_grad[None],
        grad_out_proj,
        d_gate,
        d_drive,
        d_log_decay,
    )


def solution(mesh):
    in_specs = (
        P("sp", None),
        P("sp", None),
        P("sp", None),
        P("sp", None),
        P("sp", "tp"),
        P("sp", "tp"),
        P("sp", "tp"),
        P("tp", None),
        P("sp", None, "tp"),
        P("sp", None, "tp"),
        P("sp", "tp", None),
    )
    out_specs = (
        P("sp", None, "tp"),
        P("sp", None, "tp"),
        P("sp", "tp", None),
        P("sp", "tp"),
        P("sp", "tp"),
        P("sp", "tp"),
        P("sp", "tp"),
    )
    return jax.shard_map(
        on_device, mesh=mesh, in_specs=in_specs, out_specs=out_specs, check_vma=False
    )
```
